256 devices in a mesh: kv: 32 (over z, y), tp: 8 (over x, core).
Axes of the slice: x: 4, y: 4, z: 8, core: 2. Of those that a mesh axis runs over, the one named last changes fastest.
Arguments:
- tokens: bfloat16 [16, 4096], P(None, ('kv', 'tp')), may hold values from -17 to 17
- first_gain: float32 [4096], P('kv'), may hold values from 0.1 to 1.9
- first_gate: bfloat16 [4096, 11264], P('kv', 'tp'), may hold values from -0.09375 to 0.09375
- first_up: bfloat16 [4096, 11264], P('kv', 'tp'), may hold values from -0.09375 to 0.09375
- first_down: bfloat16 [11264, 4096], P('tp', 'kv'), may hold values from -0.0546875 to 0.0546875
- mixer_gain: float32 [4096], P('kv'), may hold values from 0.1 to 1.9
- w_query: bfloat16 [4096, 4096], P('kv', 'tp'), may hold values from -0.09375 to 0.09375
- w_key: bfloat16 [4096, 4096], P('kv', 'tp'), may hold values from -0.328125 to 0.328125
- w_value: bfloat16 [4096, 4096], P('kv', 'tp'), may hold values from -0.09375 to 0.09375
- w_output: bfloat16 [4096, 4096], P('tp', 'kv'), may hold values from -0.09375 to 0.09375
- lam_heads: float32 [32], P('tp'), may hold values from 0.3 to 0.8
- head_gain: float32 [128], replicated, may hold values from 0.1 to 1.9
- key_cache: bfloat16 [16, 8192, 32, 128], P(None, 'kv', 'tp'), may hold values from -1000 to 1000
- value_cache: bfloat16 [16, 8192, 32, 128], P(None, 'kv', 'tp'), may hold values from -6 to 6
- lengths: int32 [16], replicated, may hold values from 1 to 8192, 49152 in all
- last_gain: float32 [4096], P('kv'), may hold values from 0.1 to 1.9
- last_gate: bfloat16 [4096, 11264], P('kv', 'tp'), may hold values from -0.09375 to 0.09375
- last_up: bfloat16 [4096, 11264], P('kv', 'tp'), may hold values from -0.09375 to 0.09375
- last_down: bfloat16 [11264, 4096], P('tp', 'kv'), may hold values from -0.0546875 to 0.0546875
Outputs:
- result: bfloat16 [16, 4096], P(None, ('kv', 'tp'))
The draws below stay inside these ranges and needn't reach their ends.
Inputs may be any that keep to these rules, and one draw needn't show every extreme that they name: Sequence b reads cached positions 0 to lengths[b] - 1 and its new token.
All inputs are finite; a program needn't handle non-finite values.
Results may differ from the reference program's by a relative error of at most 0.04.
Values may be sent and summed in bfloat16 or wider, within the bound.
A program may use at most 64 MiB of HBM per device.

```python
import math
import jax
import jax.numpy as jnp
import numpy as np
from jax import lax

WIDTH = 4096
HEADS = 32
HEAD_DIM = 64
VAL_DIM = 128
FFN_UNITS = 11264
BATCH = 16
SEQ_LEN = 8192


def draw_tokens(key, part):
    base = jnp.clip(jax.random.normal(jax.random.fold_in(key, 11), (BATCH, WIDTH), jnp.float32), -6.0, 6.0)
    column = jnp.arange(WIDTH, dtype=jnp.float32) / (WIDTH - 1)
    logit_scale = 0.6 * jnp.exp(jnp.log(4.0) * column)[None, :]
    return (base * logit_scale).astype(jnp.bfloat16)


def draw_key_cache(key, part):
    shape = (BATCH, SEQ_LEN, HEADS, 2 * HEAD_DIM)
    base = 1.75 * jnp.clip(jax.random.normal(jax.random.fold_in(key, 21), shape, jnp.float32), -8.0, 8.0)
    return base.astype(jnp.bfloat16)


def block_levels(rng, dims, split, low, top_value):
    def one(axis_at, parts):
        steps = jax.random.uniform(jax.random.fold_in(jax.random.fold_in(rng, 6), axis_at), (parts,), jnp.float32, low / len(split), top_value / len(split))
        return jnp.repeat(jnp.exp(steps), dims[axis_at] // parts).reshape((-1,) + (1,) * (len(dims) - axis_at - 1))

    loudness = one(*split[0])
    for cut in split[1:]:
        loudness = loudness * one(*cut)
    return loudness


def length_profile(count, total, reach, slope):
    weights = [(1 << 20) // math.isqrt(standing ** slope) + 1 for standing in range(2, count + 1)]
    spare, counts = total - reach - (count - 1), [1] * (count - 1)
    while spare > 0:
        movable = [i for i in range(count - 1) if counts[i] < reach]
        mass, budget = sum([weights[i] for i in movable]), spare
        for i in movable:
            addition = min(reach - counts[i], max(1, budget * weights[i] // mass), spare)
            counts[i] = counts[i] + addition
            spare = spare - addition
    return np.array([reach] + counts)


def uneven_parts(key, amount, total, bound, slope):
    if amount == 2:
        one = jax.random.randint(key, (), max(1, total - bound), min(bound, total - 1) + 1)
        return jnp.stack([one, total - one])
    sizes = jnp.asarray(length_profile(amount, total, bound, slope), jnp.int32)
    pairs = (amount - 1) // 2
    giver, sink = sizes[1:1 + 2 * pairs:2], sizes[2:2 + 2 * pairs:2]
    slack = jnp.minimum(giver - 1, bound - sink)
    moved = jax.random.randint(jax.random.fold_in(key, 1), (pairs,), 0, 1 << 20) % (slack + 1)
    sizes = sizes.at[1:1 + 2 * pairs:2].set(giver - moved).at[2:2 + 2 * pairs:2].set(sink + moved)
    return sizes[jax.random.permutation(jax.random.fold_in(key, 2), amount)]


def noise(key, shape, deviation, limit, cuts=(), kind=jnp.bfloat16):
    result = deviation * jax.random.normal(key, shape, jnp.float32)
    if cuts:
        result = result * block_levels(key, shape, cuts, -0.22, 0.18)
    return jnp.clip(result, -limit, limit).astype(kind)


def setup_inputs(seed: int = 0) -> dict:
    streams_of = jax.random.split(jax.random.key(seed), 20)
    return {
        "tokens": draw_tokens(jax.random.fold_in(streams_of[19], 71), 0),
        "first_gain": jnp.clip(1.0 + 0.18 * jax.random.normal(streams_of[1], (WIDTH,), jnp.float32), 0.1, 1.9),
        "first_gate": noise(streams_of[2], (WIDTH, FFN_UNITS), WIDTH ** -0.5, 0.09375, ((0, 32), (1, 8))),
        "first_up": noise(streams_of[3], (WIDTH, FFN_UNITS), WIDTH ** -0.5, 0.09375, ((0, 32), (1, 8))),
        "first_down": noise(streams_of[4], (FFN_UNITS, WIDTH), FFN_UNITS ** -0.5, 0.0546875, ((0, 8), (1, 32))),
        "mixer_gain": jnp.clip(1.0 + 0.18 * jax.random.normal(streams_of[5], (WIDTH,), jnp.float32), 0.1, 1.9),
        "w_query": noise(streams_of[6], (WIDTH, HEADS * 2 * HEAD_DIM), WIDTH ** -0.5, 0.09375, ((0, 32), (1, 8))),
        "w_key": noise(streams_of[7], (WIDTH, HEADS * 2 * HEAD_DIM), (3.5 / WIDTH ** 0.5), 0.328125, ((0, 32), (1, 8))),
        "w_value": noise(streams_of[8], (WIDTH, HEADS * VAL_DIM), WIDTH ** -0.5, 0.09375, ((0, 32), (1, 8))),
        "w_output": noise(streams_of[9], (HEADS * VAL_DIM, WIDTH), (HEADS * VAL_DIM) ** -0.5, 0.09375, ((0, 8), (1, 32))),
        "lam_heads": jnp.clip(0.3 + 0.5 * jax.random.uniform(streams_of[10], (HEADS,), jnp.float32) ** block_levels(streams_of[10], (HEADS,), ((0, 8),), -0.2, 0.2), 0.3, 0.8),
        "head_gain": jnp.clip(1.0 + 0.18 * jax.random.normal(streams_of[11], (VAL_DIM,), jnp.float32), 0.1, 1.9),
        "key_cache": draw_key_cache(jax.random.fold_in(streams_of[19], 71), 0),
        "value_cache": noise(streams_of[13], (BATCH, SEQ_LEN, HEADS, VAL_DIM), 1.0, 6.0, ((1, 32), (2, 8))),
        "lengths": uneven_parts(streams_of[14], BATCH, 3 * SEQ_LEN * BATCH // 8, SEQ_LEN, 2).astype(jnp.int32),
        "last_gain": jnp.clip(1.0 + 0.18 * jax.random.normal(streams_of[15], (WIDTH,), jnp.float32), 0.1, 1.9),
        "last_gate": noise(streams_of[16], (WIDTH, FFN_UNITS), WIDTH ** -0.5, 0.09375, ((0, 32), (1, 8))),
        "last_up": noise(streams_of[17], (WIDTH, FFN_UNITS), WIDTH ** -0.5, 0.09375, ((0, 32), (1, 8))),
        "last_down": noise(streams_of[18], (FFN_UNITS, WIDTH), FFN_UNITS ** -0.5, 0.0546875, ((0, 8), (1, 32))),
    }


epsilon = 1e-06
neg_fill = -1e+30

def gated_units(stream, gain, gate_w, up_w, down_w):
    wide = stream.astype(jnp.float32)
    inv_rms = lax.rsqrt(lax.optimization_barrier(jnp.mean(wide * wide, axis=1, keepdims=True)) + epsilon)
    scaled = (wide * gain).astype(jnp.bfloat16)
    gate_pre = jnp.dot(scaled, gate_w, preferred_element_type=jnp.float32) * inv_rms
    up_pre = jnp.dot(scaled, up_w, preferred_element_type=jnp.float32) * inv_rms
    hidden_act = (jax.nn.silu(gate_pre) * up_pre).astype(jnp.bfloat16)
    return jnp.dot(hidden_act, down_w, preferred_element_type=jnp.float32)

def one_sequence(items):
    query_rows, keys, values, length, fresh_key, new_value, lam_heads = items
    seq_len = keys.shape[0]
    logit_scale = HEAD_DIM ** (-0.5)
    query_single32 = query_rows.astype(jnp.float32)
    key_entries = keys.astype(jnp.float32).reshape(seq_len, HEADS, 2, HEAD_DIM)
    score_matrix = jnp.einsum('fuz,tfuz->fut', query_single32, key_entries) * logit_scale
    positions = jnp.arange(seq_len, dtype=jnp.int32)
    live_mask = (positions < length)[None, None, :]
    score_matrix = jnp.where(live_mask, score_matrix, neg_fill)
    self_score = jnp.einsum('vij,vij->vi', query_single32, fresh_key.astype(jnp.float32)) * logit_scale
    highest = jnp.maximum(lax.optimization_barrier(jnp.max(score_matrix, axis=-1)), self_score)
    weights = jnp.where(live_mask, jnp.exp(score_matrix - highest[..., None]), 0.0)
    own_weight = jnp.exp(self_score - highest)
    totals = lax.optimization_barrier(jnp.sum(weights, axis=-1)) + own_weight
    rounded = lax.optimization_barrier(weights.astype(jnp.bfloat16)).astype(jnp.float32)
    own_round = lax.optimization_barrier(own_weight.astype(jnp.bfloat16)).astype(jnp.float32)
    weighted = jnp.einsum('hml,lhe->hme', rounded, values.astype(jnp.float32))
    weighted = weighted + own_round[..., None] * new_value.astype(jnp.float32)[:, None, :]
    return weighted[:, 0] / totals[:, 0, None] - lam_heads[:, None] * weighted[:, 1] / totals[:, 1, None]

def reference(tokens, first_gain, first_gate, first_up, first_down, mixer_gain, w_query, w_key, w_value, w_output, lam_heads, head_gain, key_cache, value_cache, lengths, last_gain, last_gate, last_up, last_down):
    batch = tokens.shape[0]
    first = (tokens.astype(jnp.float32) + 0.5 * gated_units(tokens, first_gain, first_gate, first_up, first_down)).astype(jnp.bfloat16)
    wide = first.astype(jnp.float32)
    inv_rms = lax.rsqrt(lax.optimization_barrier(jnp.mean(wide * wide, axis=1, keepdims=True)) + epsilon)
    scaled = (wide * mixer_gain).astype(jnp.bfloat16)
    query_rows = (jnp.dot(scaled, w_query, preferred_element_type=jnp.float32) * inv_rms).astype(jnp.bfloat16)
    fresh_key = (jnp.dot(scaled, w_key, preferred_element_type=jnp.float32) * inv_rms).astype(jnp.bfloat16)
    new_value = (jnp.dot(scaled, w_value, preferred_element_type=jnp.float32) * inv_rms).astype(jnp.bfloat16)
    query_rows = query_rows.reshape(batch, HEADS, 2, HEAD_DIM)
    fresh_key = fresh_key.reshape(batch, HEADS, 2, HEAD_DIM)
    new_value = new_value.reshape(batch, HEADS, VAL_DIM)
    lam_rows = jnp.broadcast_to(lam_heads, (batch, HEADS))
    mixed = lax.map(one_sequence, (query_rows, key_cache, value_cache, lengths, fresh_key, new_value, lam_rows))
    normed = mixed * lax.rsqrt(lax.optimization_barrier(jnp.mean(mixed * mixed, axis=-1, keepdims=True)) + epsilon) * head_gain
    attended = normed.astype(jnp.bfloat16).reshape(batch, HEADS * VAL_DIM)
    projected = jnp.dot(attended, w_output, preferred_element_type=jnp.float32)
    second = (wide + projected).astype(jnp.bfloat16)
    last = gated_units(second, last_gain, last_gate, last_up, last_down)
    return (second.astype(jnp.float32) + 0.5 * last).astype(jnp.bfloat16)
```

```python
import functools

import jax
import jax.numpy as jnp
from jax import lax
from jax.experimental import pallas as pl
from jax.experimental.pallas import tpu as pltpu
from jax.sharding import PartitionSpec as P

HEAD_DIM = 64
LANES = 128
MAPS = 2
EPSILON = 1e-06
NEG = -1e30
MESH = pl.DeviceIdType.MESH
F32 = jnp.float32
BF16 = jnp.bfloat16


def owner_of(b):
    return 4 * (b // 2) + 2 * (b % 2) + (b // 2) % 2


def split_in_two(value):
    high = value.astype(BF16).astype(F32)
    return high, value - high


def layer_kernel(
    dims,
    tokens,
    first_gain,
    mixer_gain,
    last_gain,
    head_gain,
    lam,
    lengths,
    first_gate,
    first_up,
    first_down,
    w_query,
    w_key,
    w_value,
    w_output,
    key_cache,
    value_cache,
    last_gate,
    last_up,
    last_down,
    result,
    v_gate1,
    v_up1,
    v_down1,
    v_query,
    v_key,
    v_value,
    v_output,
    v_keys,
    v_values,
    v_gate2,
    v_up2,
    v_down2,
    load_sem,
    tp_slots,
    tp_send,
    tp_recv,
    blocks,
    rows_f32,
    ffn_out,
    ffn_in,
    qkv_out,
    qkv_in,
    att_out,
    att_in,
    hid_all,
    query_all,
    head_all,
    own_rows,
    out_send,
    in_recv,
    all_send,
    all_recv,
):
    KV, TP, B, NH, FB, POS, WIDTH = dims
    FH = FB + 1
    k = lax.axis_index("kv")
    t = lax.axis_index("tp")
    is_owner = lax.rem(k, 2) == lax.rem(k // 4, 2)
    mine = k // 2

    loads = [
        (first_gate, v_gate1),
        (first_up, v_up1),
        (first_down, v_down1),
        (w_query, v_query),
        (w_key, v_key),
        (w_value, v_value),
        (key_cache, v_keys),
        (value_cache, v_values),
        (w_output, v_output),
        (last_gate, v_gate2),
        (last_up, v_up2),
        (last_down, v_down2),
    ]
    copies = [pltpu.make_async_copy(src, dst, load_sem.at[i]) for i, (src, dst) in enumerate(loads)]

    barrier = pltpu.get_barrier_semaphore()

    def greet_kv(d, _):
        pl.semaphore_signal(barrier, inc=1, device_id={"kv": lax.rem(k + d, KV)}, device_id_type=MESH)
        return 0

    def greet_tp(d, _):
        pl.semaphore_signal(barrier, inc=1, device_id={"tp": lax.rem(t + d, TP)}, device_id_type=MESH)
        return 0

    lax.fori_loop(1, KV, greet_kv, 0)
    lax.fori_loop(1, TP, greet_tp, 0)
    for copy in copies:
        copy.start()
    pl.semaphore_wait(barrier, KV - 1 + TP - 1)

    def tp_copy(turn, d):
        return pltpu.make_async_remote_copy(
            src_ref=tp_slots.at[turn, t],
            dst_ref=tp_slots.at[turn, t],
            send_sem=tp_send.at[turn, d],
            recv_sem=tp_recv.at[turn, d],
            device_id={"tp": lax.rem(t + d, TP)},
            device_id_type=MESH,
        )

    def tp_sum(turn, value):
        tp_slots[turn, t] = value

        def send(d, _):
            tp_copy(turn, d).start()
            return 0

        def take(d, _):
            tp_copy(turn, d).wait()
            return 0

        lax.fori_loop(1, TP, send, 0)
        lax.fori_loop(1, TP, take, 0)
        total = tp_slots[turn, 0]
        for s in range(1, TP):
            total = total + tp_slots[turn, s]
        return total

    def out_copy(turn, b, source, out_ref, in_ref):
        return pltpu.make_async_remote_copy(
            src_ref=out_ref.at[b],
            dst_ref=in_ref.at[source],
            send_sem=out_send.at[turn, b],
            recv_sem=in_recv.at[turn, source],
            device_id={"kv": owner_of(b)},
            device_id_type=MESH,
        )

    def send_row(turn, b, out_ref, in_ref):
        there = owner_of(b)

        @pl.when(there != k)
        def _():
            out_copy(turn, b, k, out_ref, in_ref).start()

        @pl.when(there == k)
        def _():
            in_ref[k] = out_ref[b]

    def send_rows(turn, out_ref, in_ref):
        def send(i, _):
            send_row(turn, lax.rem(mine + B // 2 + i, B), out_ref, in_ref)
            return 0

        lax.fori_loop(0, B, send, 0)

    def take_rows(turn, out_ref, in_ref):
        def take(d, _):
            out_copy(turn, mine, lax.rem(k + d, KV), out_ref, in_ref).wait_recv()
            return 0

        lax.fori_loop(1, KV, take, 0)

    def all_copy(turn, b, d, ref):
        return pltpu.make_async_remote_copy(
            src_ref=ref.at[b],
            dst_ref=ref.at[b],
            send_sem=all_send.at[turn, d],
            recv_sem=all_recv.at[turn, b],
            device_id={"kv": lax.rem(k + d, KV)},
            device_id_type=MESH,
        )

    def share_row(turn, ref):
        def send(i, _):
            d = 1 + lax.rem(i + KV // 2 - 1, KV - 1)
            all_copy(turn, mine, d, ref).start()
            return 0

        lax.fori_loop(0, KV - 1, send, 0)

    def take_all(turn, ref):
        def take(b, _):
            @pl.when(owner_of(b) != k)
            def _():
                all_copy(turn, b, 1, ref).wait_recv()

            return 0

        lax.fori_loop(0, B, take, 0)

    def as_lhs(ref, count):
        rows = ref.shape[1]
        rows_f32[0 : B * rows, :] = ref[...].astype(F32).reshape(B * rows, LANES)
        parts = [rows_f32[pl.ds(c, B, stride=rows), :] for c in range(count)]
        return jnp.concatenate(parts, axis=1).astype(BF16)

    def put_block(c, value):
        blocks[c * B : (c + 1) * B, :] = value

    def pack_rows(count, out_ref):
        for b in range(B):
            out_ref[b] = blocks[pl.ds(b, count, stride=B), :].astype(BF16)

    def normed_rows(stream, gain):
        squares = jnp.sum(stream * stream, axis=1, keepdims=True)
        high, low = split_in_two(jnp.broadcast_to(squares, (B, LANES)))
        return (stream * gain[...]).astype(BF16), high, low

    def gated_units(turn, stream, gain, gate_w, up_w, down_w, waits):
        scaled, high, low = normed_rows(stream, gain)
        put_block(FB, high)
        put_block(FH + FB, low)
        for at, weight, wait in ((0, gate_w, waits[0]), (FH, up_w, waits[1])):
            wait.wait()
            part = jnp.dot(scaled, weight[...], preferred_element_type=F32)
            for c in range(FB):
                put_block(at + c, part[:, c * LANES : (c + 1) * LANES])
        out_ref, in_ref = ffn_out.at[turn], ffn_in.at[turn]
        hid_ref = hid_all.at[turn]
        pack_rows(2 * FH, out_ref)
        send_rows(3 * turn, out_ref, in_ref)

        @pl.when(is_owner)
        def _():
            take_rows(3 * turn, out_ref, in_ref)
            total = jnp.sum(in_ref[...].astype(F32), axis=0)
            squares = total[FB : FB + 1] + total[FH + FB : FH + FB + 1]
            inv = lax.rsqrt(squares / WIDTH + EPSILON)
            gate = total[0:FH] * inv
            up = total[FH : 2 * FH] * inv
            hid = jax.nn.silu(gate) * up
            hid = jnp.where(lax.broadcasted_iota(jnp.int32, hid.shape, 0) < FB, hid, 0.0)
            pad = hid_ref.shape[1] - FH
            hid_ref[mine] = jnp.concatenate([hid, jnp.zeros((pad, LANES), F32)], axis=0).astype(BF16)
            share_row(3 * turn, hid_ref)

        take_all(3 * turn, hid_ref)
        hidden = as_lhs(hid_ref, FB)
        waits[2].wait()
        return jnp.dot(hidden, down_w[...], preferred_element_type=F32)

    tokens_f32 = tokens[...].astype(F32)
    columns = tokens_f32.shape[1]
    wide = jnp.concatenate([tokens_f32, jnp.zeros((B, LANES - columns), F32)], axis=1)
    stream = tp_sum(0, pltpu.roll(wide, t * columns, 1))

    part = gated_units(0, stream, first_gain, v_gate1, v_up1, v_down1, copies[0:3])
    first = (stream + 0.5 * tp_sum(1, part)).astype(BF16).astype(F32)

    scaled, high, low = normed_rows(first, mixer_gain)
    for n, weight in enumerate((v_query, v_key, v_value)):
        copies[3 + n].wait()
        part = jnp.dot(scaled, weight[...], preferred_element_type=F32)
        for c in range(NH):
            put_block(NH * n + c, part[:, c * LANES : (c + 1) * LANES])
    put_block(3 * NH, high)
    put_block(3 * NH + 1, low)
    put_block(3 * NH + 2, jnp.zeros((B, LANES), F32))
    put_block(3 * NH + 3, jnp.zeros((B, LANES), F32))
    pack_rows(4 * NH, qkv_out)
    send_rows(1, qkv_out, qkv_in)

    @pl.when(is_owner)
    def _():
        take_rows(1, qkv_out, qkv_in)
        total = jnp.sum(qkv_in[...].astype(F32), axis=0)
        squares = total[3 * NH : 3 * NH + 1] + total[3 * NH + 1 : 3 * NH + 2]
        inv = lax.rsqrt(squares / WIDTH + EPSILON)
        rows = (total[0 : 3 * NH] * inv).astype(BF16).astype(F32)
        query, new_key, new_value = rows[0:NH], rows[NH : 2 * NH], rows[2 * NH : 3 * NH]
        first_map = lax.broadcasted_iota(jnp.int32, (NH, LANES), 1) < HEAD_DIM
        query = query * HEAD_DIM ** (-0.5)
        both = jnp.concatenate(
            [jnp.where(first_map, query, 0.0), jnp.where(first_map, 0.0, query)], axis=0
        )
        query_all[mine] = both.astype(BF16)
        share_row(1, query_all)
        own = jnp.sum(both * jnp.concatenate([new_key, new_key], axis=0), axis=1, keepdims=True)
        own_rows[0] = jnp.broadcast_to(own, (MAPS * NH, LANES))
        own_rows[1] = jnp.concatenate([new_value, new_value], axis=0)

    take_all(1, query_all)

    copies[6].wait()
    copies[7].wait()
    span = POS * NH
    row = lax.broadcasted_iota(jnp.int32, (MAPS * NH, span), 0)
    lane = lax.broadcasted_iota(jnp.int32, (MAPS * NH, span), 1)
    own_head = lax.rem(lane, NH) == lax.rem(row, NH)
    position = k * POS + lane // NH
    stat_lane = lax.broadcasted_iota(jnp.int32, (MAPS * NH, LANES), 1)

    def attend(i, _):
        b = lax.rem(mine + B // 2 + i, B)
        scores = lax.dot_general(
            query_all[b], v_keys[b], (((1,), (1,)), ((), ())), preferred_element_type=F32
        )
        live = jnp.logical_and(own_head, position < lengths[b])
        scores = jnp.where(live, scores, NEG)
        peak_high, peak_low = split_in_two(jnp.max(scores, axis=1, keepdims=True))
        peak_low = peak_low.astype(BF16).astype(F32)
        weights = jnp.where(live, jnp.exp(scores - (peak_high + peak_low)), 0.0)
        den_high, den_low = split_in_two(jnp.sum(weights, axis=1, keepdims=True))
        num = jnp.dot(weights.astype(BF16), v_values[b], preferred_element_type=F32)
        stats = jnp.where(
            stat_lane < 64,
            jnp.where(stat_lane < 32, peak_high, peak_low),
            jnp.where(stat_lane < 96, den_high, den_low),
        )
        att_out[b] = jnp.concatenate([num, stats], axis=0).astype(BF16)
        send_row(2, b, att_out, att_in)
        return 0

    lax.fori_loop(0, B, attend, 0)

    @pl.when(is_owner)
    def _():
        take_rows(2, att_out, att_in)
        arrived = att_in[...].astype(F32)
        num, stats = arrived[:, 0 : MAPS * NH], arrived[:, MAPS * NH : 2 * MAPS * NH]
        peak = stats[:, :, 0:1] + stats[:, :, 32:33]
        den = stats[:, :, 64:65] + stats[:, :, 96:97]
        own = own_rows[0][:, 0:1]
        highest = jnp.maximum(jnp.max(peak, axis=0), own)
        scale = jnp.exp(peak - highest[None])
        own_weight = jnp.exp(own - highest)
        own_round = own_weight.astype(BF16).astype(F32)
        total = jnp.sum(scale * den, axis=0) + own_weight
        weighted = jnp.sum(scale * num, axis=0) + own_round * own_rows[1]
        mixed = weighted / total
        head = lax.broadcasted_iota(jnp.int32, (NH, 1), 0)
        lam_rows = jnp.zeros((NH, 1), F32)
        for h in range(NH):
            lam_rows = jnp.where(head == h, lam[h], lam_rows)
        mixed = mixed[0:NH] - lam_rows * mixed[NH : 2 * NH]
        inv = lax.rsqrt(jnp.mean(mixed * mixed, axis=1, keepdims=True) + EPSILON)
        normed = mixed * inv * head_gain[...]
        head_all[mine] = jnp.concatenate([normed, jnp.zeros((NH, LANES), F32)], axis=0).astype(BF16)
        share_row(2, head_all)

    take_all(2, head_all)
    attended = as_lhs(head_all, NH)
    copies[8].wait()
    part = jnp.dot(attended, v_output[...], preferred_element_type=F32)
    second = (first + tp_sum(2, part)).astype(BF16).astype(F32)

    part = gated_units(1, second, last_gain, v_gate2, v_up2, v_down2, copies[9:12])
    last = second + 0.5 * tp_sum(3, part)
    own_columns = lax.rem(LANES - t * columns, LANES)
    result[...] = pltpu.roll(last, own_columns, 1)[:, 0:columns].astype(BF16)

    def sent_rows(turn, out_ref, in_ref):
        def sent(b, _):
            @pl.when(owner_of(b) != k)
            def _():
                out_copy(turn, b, k, out_ref, in_ref).wait_send()

            return 0

        lax.fori_loop(0, B, sent, 0)

    def sent_all(turn, ref):
        @pl.when(is_owner)
        def _():
            def sent(d, _):
                all_copy(turn, mine, d, ref).wait_send()
                return 0

            lax.fori_loop(1, KV, sent, 0)

    sent_rows(0, ffn_out.at[0], ffn_in.at[0])
    sent_rows(1, qkv_out, qkv_in)
    sent_rows(2, att_out, att_in)
    sent_rows(3, ffn_out.at[1], ffn_in.at[1])
    sent_all(0, hid_all.at[0])
    sent_all(1, query_all)
    sent_all(2, head_all)
    sent_all(3, hid_all.at[1])


def on_device(KV, TP):
    def run(
        tokens,
        first_gain,
        first_gate,
        first_up,
        first_down,
        mixer_gain,
        w_query,
        w_key,
        w_value,
        w_output,
        lam_heads,
        head_gain,
        key_cache,
        value_cache,
        lengths,
        last_gain,
        last_gate,
        last_up,
        last_down,
    ):
        B, POS, NH, _ = key_cache.shape
        FB = first_gate.shape[1] // LANES
        FH = FB + 1
        HR = -(-FH // 8) * 8
        WIDTH = w_query.shape[0] * KV
        dims = (KV, TP, B, NH, FB, POS, WIDTH)
        vmem = pl.BlockSpec(memory_space=pltpu.VMEM)
        smem = pl.BlockSpec(memory_space=pltpu.SMEM)
        far = pl.BlockSpec(memory_space=pl.ANY)
        flat_keys = key_cache.reshape(B, POS * NH, LANES)
        flat_values = value_cache.reshape(B, POS * NH, LANES)
        large = (first_gate, first_up, first_down, w_query, w_key, w_value, w_output)
        large += (flat_keys, flat_values, last_gate, last_up, last_down)
        return pl.pallas_call(
            functools.partial(layer_kernel, dims),
            out_shape=jax.ShapeDtypeStruct(tokens.shape, BF16),
            in_specs=[vmem] * 5 + [smem] * 2 + [far] * 12,
            out_specs=vmem,
            scratch_shapes=[
                *(pltpu.VMEM(a.shape, a.dtype) for a in large),
                pltpu.SemaphoreType.DMA((12,)),
                pltpu.VMEM((4, TP, B, LANES), F32),
                pltpu.SemaphoreType.DMA((4, TP)),
                pltpu.SemaphoreType.DMA((4, TP)),
                pltpu.VMEM((max(2 * FH, 4 * NH) * B, LANES), F32),
                pltpu.VMEM((max(HR, 2 * NH) * B, LANES), F32),
                pltpu.VMEM((2, B, 2 * FH, LANES), BF16),
                pltpu.VMEM((2, KV, 2 * FH, LANES), BF16),
                pltpu.VMEM((B, 4 * NH, LANES), BF16),
                pltpu.VMEM((KV, 4 * NH, LANES), BF16),
                pltpu.VMEM((B, 4 * NH, LANES), BF16),
                pltpu.VMEM((KV, 4 * NH, LANES), BF16),
                pltpu.VMEM((2, B, HR, LANES), BF16),
                pltpu.VMEM((B, 2 * NH, LANES), BF16),
                pltpu.VMEM((B, 2 * NH, LANES), BF16),
                pltpu.VMEM((2, 2 * NH, LANES), F32),
                pltpu.SemaphoreType.DMA((4, B)),
                pltpu.SemaphoreType.DMA((4, KV)),
                pltpu.SemaphoreType.DMA((4, KV)),
                pltpu.SemaphoreType.DMA((4, B)),
            ],
            compiler_params=pltpu.CompilerParams(collective_id=0, has_side_effects=True),
        )(
            tokens,
            first_gain.reshape(1, LANES),
            mixer_gain.reshape(1, LANES),
            last_gain.reshape(1, LANES),
            head_gain.reshape(1, LANES),
            lam_heads,
            lengths,
            first_gate,
            first_up,
            first_down,
            w_query,
            w_key,
            w_value,
            w_output,
            flat_keys,
            flat_values,
            last_gate,
            last_up,
            last_down,
        )

    return run


def solution(mesh):
    return jax.shard_map(
        on_device(mesh.shape["kv"], mesh.shape["tp"]),
        mesh=mesh,
        in_specs=(
            P(None, ("kv", "tp")),
            P("kv"),
            P("kv", "tp"),
            P("kv", "tp"),
            P("tp", "kv"),
            P("kv"),
            P("kv", "tp"),
            P("kv", "tp"),
            P("kv", "tp"),
            P("tp", "kv"),
            P("tp"),
            P(),
            P(None, "kv", "tp", None),
            P(None, "kv", "tp", None),
            P(),
            P("kv"),
            P("kv", "tp"),
            P("kv", "tp"),
            P("tp", "kv"),
        ),
        out_specs=P(None, ("kv", "tp")),
        check_vma=False,
    )
```

```python
import functools

import jax
import jax.numpy as jnp
from jax import lax
from jax.experimental import pallas as pl
from jax.experimental.pallas import tpu as pltpu
from jax.sharding import PartitionSpec as P

HEAD_DIM = 64
LANES = 128
MAPS = 2
EPSILON = 1e-06
NEG = -(2.0**100)
MESH = pl.DeviceIdType.MESH
F32 = jnp.float32
BF16 = jnp.bfloat16


def server_of(b, t):
    z = b // 2
    return 4 * z + 2 * lax.rem(b, 2) + lax.rem(z + 1 + t, 2), t + 1 - lax.rem(t, 2)


def split_in_two(value):
    high = value.astype(BF16).astype(F32)
    return high, value - high


def layer_kernel(
    dims,
    tokens,
    first_gain,
    mixer_gain,
    last_gain,
    head_gain,
    lam,
    lengths,
    first_gate,
    first_up,
    first_down,
    w_query,
    w_key,
    w_value,
    w_output,
    key_cache,
    value_cache,
    last_gate,
    last_up,
    last_down,
    result,
    v_gate1,
    v_up1,
    v_down1,
    v_query,
    v_key,
    v_value,
    v_output,
    v_keys,
    v_values,
    v_gate2,
    v_up2,
    v_down2,
    v_tokens,
    v_gain1,
    v_gain2,
    v_gain3,
    v_head_gain,
    load_sem,
    tp_slots,
    tp_send,
    tp_recv,
    blocks,
    rows_f32,
    ffn_out,
    ffn_in,
    qkv_out,
    qkv_in,
    att_out,
    att_in,
    hid_row,
    hid_all,
    query_row,
    query_all,
    head_row,
    head_all,
    own_rows,
    long_rows,
    short_rows,
    out_send,
    in_recv,
    all_send,
    all_recv,
):
    KV, TP, B, NH, FB, POS, WIDTH = dims
    FH = FB + 1
    Y, Z = 4, KV // 4
    k = lax.axis_index("kv")
    t = lax.axis_index("tp")
    mine = k // 2
    serves = lax.rem(t, 2) == 1
    group = t - lax.rem(k + k // 4, 2)
    home = jnp.logical_and(serves, group == t)
    away = jnp.logical_and(serves, group != t)

    loads = [
        (first_gate, v_gate1),
        (first_up, v_up1),
        (first_down, v_down1),
        (w_query, v_query),
        (w_key, v_key),
        (w_value, v_value),
        (key_cache, v_keys),
        (value_cache, v_values),
        (w_output, v_output),
        (last_gate, v_gate2),
        (last_up, v_up2),
        (last_down, v_down2),
        (tokens, v_tokens),
        (first_gain, v_gain1),
        (mixer_gain, v_gain2),
        (last_gain, v_gain3),
        (head_gain, v_head_gain),
    ]
    copies = [pltpu.make_async_copy(src, dst, load_sem.at[i]) for i, (src, dst) in enumerate(loads)]

    def from_far(i, size):
        half = (i + 1) // 2
        return lax.rem(size // 2 + half * (1 - 2 * lax.rem(i, 2)), size)

    def kv_from_far(i):
        z = lax.rem(k // Y + from_far(i // Y, Z), Z)
        y = lax.rem(lax.rem(k, Y) + from_far(lax.rem(i, Y), Y), Y)
        return z * Y + y

    def row_from_far(i):
        z = lax.rem(k // Y + from_far(i // 2, Z), Z)
        return 2 * z + lax.rem(mine + 1 + i, 2)

    barrier = pltpu.get_barrier_semaphore()

    def greet(kv, tp):
        pl.semaphore_signal(barrier, inc=1, device_id={"kv": kv, "tp": tp}, device_id_type=MESH)

    def greet_server(i, _):
        b = row_from_far(i)

        @pl.when(jnp.logical_not(jnp.logical_and(home, b == mine)))
        def _():
            greet(*server_of(b, t))

        return 0

    def greet_group(i, _):
        there = kv_from_far(i)

        @pl.when(jnp.logical_not(jnp.logical_and(home, there == k)))
        def _():
            greet(there, group)

        return 0

    def greet_tp(d, _):
        greet(k, lax.rem(t + d, TP))
        return 0

    with jax.named_scope("greet"):

        @pl.when(serves)
        def _():
            lax.fori_loop(0, KV, greet_group, 0)

        lax.fori_loop(0, B, greet_server, 0)
        lax.fori_loop(1, TP, greet_tp, 0)
    for copy in copies[12:] + copies[:12]:
        copy.start()
    for copy in copies[12:]:
        copy.wait()

    with jax.named_scope("barrier"):

        @pl.when(home)
        def _():
            pl.semaphore_wait(barrier, B - 1 + KV - 1 + TP - 1)

        @pl.when(away)
        def _():
            pl.semaphore_wait(barrier, B + KV + TP - 1)

        @pl.when(jnp.logical_not(serves))
        def _():
            pl.semaphore_wait(barrier, B + TP - 1)

    def remote(src, dst, send_sem, recv_sem, kv, tp):
        return pltpu.make_async_remote_copy(
            src_ref=src,
            dst_ref=dst,
            send_sem=send_sem,
            recv_sem=recv_sem,
            device_id={"kv": kv, "tp": tp},
            device_id_type=MESH,
        )

    def all_of(ref, count, send_sem, recv_sem):
        some = ref.at[pl.ds(0, count)]
        return remote(some, some, send_sem, recv_sem, k, t)

    def tp_sum(turn, value):
        slot = tp_slots.at[turn, t]
        slot[...] = value.astype(BF16)
        send_sem, recv_sem = tp_send.at[turn], tp_recv.at[turn]

        def send(d, _):
            remote(slot, slot, send_sem, recv_sem, k, lax.rem(t + d, TP)).start()
            return 0

        with jax.named_scope(f"tp_send{turn}"):
            lax.fori_loop(1, TP, send, 0, unroll=True)
        with jax.named_scope(f"tp_take{turn}"):
            arrived = all_of(tp_slots.at[turn], TP - 1, send_sem, recv_sem)
            arrived.wait_send()
            arrived.wait_recv()
        return jnp.sum(tp_slots[turn].astype(F32), axis=0)

    def send_row(turn, b, out_ref, in_ref):
        here = jnp.logical_and(home, b == mine)

        @pl.when(jnp.logical_not(here))
        def _():
            kv, tp = server_of(b, t)
            remote(out_ref.at[b], in_ref.at[k], out_send.at[turn], in_recv.at[turn], kv, tp).start()

        @pl.when(here)
        def _():
            in_ref[k] = out_ref[b]

    def send_rows(turn, out_ref, in_ref):
        def send(i, _):
            send_row(turn, row_from_far(i), out_ref, in_ref)
            return 0

        with jax.named_scope(f"rows_send{turn}"):
            lax.fori_loop(0, B, send, 0)

    def take_rows(turn, out_ref, in_ref):
        with jax.named_scope(f"rows_take{turn}"):

            @pl.when(home)
            def _():
                all_of(in_ref, KV - 1, out_send.at[turn], in_recv.at[turn]).wait_recv()

            @pl.when(away)
            def _():
                all_of(in_ref, KV, out_send.at[turn], in_recv.at[turn]).wait_recv()

    def share_row(turn, row_ref, all_ref):
        def send(i, _):
            there = kv_from_far(i)

            @pl.when(jnp.logical_not(jnp.logical_and(home, there == k)))
            def _():
                remote(row_ref, all_ref.at[mine], all_send.at[turn], all_recv.at[turn], there, group).start()

            return 0

        with jax.named_scope(f"all_send{turn}"):
            lax.fori_loop(0, KV, send, 0)

            @pl.when(home)
            def _():
                all_ref[mine] = row_ref[...]

    def take_all(turn, out_ref, rows_ref, all_ref):
        with jax.named_scope(f"all_take{turn}"):

            @pl.when(home)
            def _():
                all_of(out_ref, B - 1, out_send.at[turn], in_recv.at[turn]).wait_send()
                all_of(rows_ref, KV - 1, all_send.at[turn], all_recv.at[turn]).wait_send()
                all_of(all_ref, B - 1, all_send.at[turn], all_recv.at[turn]).wait_recv()

            @pl.when(away)
            def _():
                all_of(rows_ref, KV, all_send.at[turn], all_recv.at[turn]).wait_send()

            @pl.when(jnp.logical_not(home))
            def _():
                all_of(out_ref, B, out_send.at[turn], in_recv.at[turn]).wait_send()
                all_of(all_ref, B, all_send.at[turn], all_recv.at[turn]).wait_recv()

    def as_lhs(ref, count):
        rows = ref.shape[1]
        rows_f32[0 : B * rows, :] = ref[...].astype(F32).reshape(B * rows, LANES)
        parts = [rows_f32[pl.ds(c, B, stride=rows), :] for c in range(count)]
        return jnp.concatenate(parts, axis=1).astype(BF16)

    def put_block(c, value):
        blocks[c * B : (c + 1) * B, :] = value

    def pack_rows(count, out_ref):
        for b in range(B):
            out_ref[b] = blocks[pl.ds(b, count, stride=B), :].astype(BF16)

    def normed_rows(stream, gain):
        squares = jnp.sum(stream * stream, axis=1, keepdims=True)
        high, low = split_in_two(jnp.broadcast_to(squares, (B, LANES)))
        return (stream * gain[...]).astype(BF16), high, low

    def gated_units(turn, stream, gain, gate_w, up_w, down_w, waits):
        scaled, high, low = normed_rows(stream, gain)
        put_block(FB, high)
        put_block(FH + FB, low)
        for at, weight, wait in ((0, gate_w, waits[0]), (FH, up_w, waits[1])):
            wait.wait()
            part = jnp.dot(scaled, weight[...], preferred_element_type=F32)
            for c in range(FB):
                put_block(at + c, part[:, c * LANES : (c + 1) * LANES])
        out_ref, in_ref = ffn_out.at[turn], ffn_in.at[turn]
        row_ref, all_ref = hid_row.at[turn], hid_all.at[turn]
        with jax.named_scope("pack"):
            pack_rows(2 * FH, out_ref)
        send_rows(3 * turn, out_ref, in_ref)

        @pl.when(serves)
        def _():
            take_rows(3 * turn, out_ref, in_ref)
            total = jnp.sum(in_ref[...].astype(F32), axis=0)
            squares = total[FB : FB + 1] + total[FH + FB : FH + FB + 1]
            inv = lax.rsqrt(squares / WIDTH + EPSILON)
            gate = total[0:FH] * inv
            up = total[FH : 2 * FH] * inv
            hid = jax.nn.silu(gate) * up
            hid = jnp.where(lax.broadcasted_iota(jnp.int32, hid.shape, 0) < FB, hid, 0.0)
            pad = row_ref.shape[0] - FH
            row_ref[...] = jnp.concatenate([hid, jnp.zeros((pad, LANES), F32)], axis=0).astype(BF16)
            share_row(3 * turn, row_ref, all_ref)

        take_all(3 * turn, out_ref, long_rows, all_ref)
        with jax.named_scope("lhs"):
            hidden = as_lhs(all_ref, FB)
        waits[2].wait()
        return jnp.dot(hidden, down_w[...], preferred_element_type=F32)

    tokens_f32 = v_tokens[...].astype(F32)
    columns = tokens_f32.shape[1]
    wide = jnp.concatenate([tokens_f32, jnp.zeros((B, LANES - columns), F32)], axis=1)
    stream = tp_sum(0, pltpu.roll(wide, t * columns, 1))

    part = gated_units(0, stream, v_gain1, v_gate1, v_up1, v_down1, copies[0:3])
    first = (stream + 0.5 * tp_sum(1, part)).astype(BF16).astype(F32)

    scaled, high, low = normed_rows(first, v_gain2)
    for n, weight in enumerate((v_query, v_key, v_value)):
        copies[3 + n].wait()
        part = jnp.dot(scaled, weight[...], preferred_element_type=F32)
        for c in range(NH):
            put_block(NH * n + c, part[:, c * LANES : (c + 1) * LANES])
    put_block(3 * NH, high)
    put_block(3 * NH + 1, low)
    section = lax.broadcasted_iota(jnp.int32, (B, LANES), 1) // (LANES // NH)
    lam_row = jnp.zeros((B, LANES), F32)
    for h in range(NH):
        lam_row = jnp.where(section == h, lam[h], lam_row)
    high, low = split_in_two(jnp.where(k == 0, lam_row, 0.0))
    put_block(3 * NH + 2, high)
    put_block(3 * NH + 3, low)
    pack_rows(4 * NH, qkv_out)
    send_rows(1, qkv_out, qkv_in)

    @pl.when(serves)
    def _():
        take_rows(1, qkv_out, qkv_in)
        total = jnp.sum(qkv_in[...].astype(F32), axis=0)
        squares = total[3 * NH : 3 * NH + 1] + total[3 * NH + 1 : 3 * NH + 2]
        inv = lax.rsqrt(squares / WIDTH + EPSILON)
        rows = (total[0 : 3 * NH] * inv).astype(BF16).astype(F32)
        query, new_key, new_value = rows[0:NH], rows[NH : 2 * NH], rows[2 * NH : 3 * NH]
        first_map = lax.broadcasted_iota(jnp.int32, (NH, LANES), 1) < HEAD_DIM
        query = query * HEAD_DIM ** (-0.5)
        both = jnp.concatenate(
            [jnp.where(first_map, query, 0.0), jnp.where(first_map, 0.0, query)], axis=0
        )
        query_row[...] = both.astype(BF16)
        share_row(1, query_row, query_all)
        own = jnp.sum(both * jnp.concatenate([new_key, new_key], axis=0), axis=1, keepdims=True)
        own_rows[0] = jnp.broadcast_to(own, (MAPS * NH, LANES))
        own_rows[1] = jnp.concatenate([new_value, new_value], axis=0)
        lam_sum = total[3 * NH + 2 : 3 * NH + 3] + total[3 * NH + 3 : 3 * NH + 4]
        own_rows[2] = jnp.broadcast_to(lam_sum, (MAPS * NH, LANES))

    take_all(1, qkv_out, short_rows, query_all)

    copies[6].wait()
    copies[7].wait()
    span = POS * NH
    row = lax.broadcasted_iota(jnp.int32, (MAPS * NH, span), 0)
    lane = lax.broadcasted_iota(jnp.int32, (MAPS * NH, span), 1)
    own_head = lax.rem(lane, NH) == lax.rem(row, NH)
    position = jnp.where(own_head, k * POS + lane // NH, KV * POS)
    stat_lane = lax.broadcasted_iota(jnp.int32, (MAPS * NH, LANES), 1)
    SIDE = 4

    def attend(i, _):
        rows_b = [row_from_far(i * SIDE + j) for j in range(SIDE)]
        scores = [
            lax.dot_general(
                query_all[b], v_keys[b], (((1,), (1,)), ((), ())), preferred_element_type=F32
            )
            for b in rows_b
        ]
        scores = [jnp.where(position < lengths[b], s, NEG) for b, s in zip(rows_b, scores)]
        peaks = [split_in_two(jnp.max(s, axis=1, keepdims=True)) for s in scores]
        peaks = [(high, low.astype(BF16).astype(F32)) for high, low in peaks]
        weights = [jnp.exp(s - (high + low)) for s, (high, low) in zip(scores, peaks)]
        nums = [
            jnp.dot(w.astype(BF16), v_values[b], preferred_element_type=F32)
            for b, w in zip(rows_b, weights)
        ]
        for b, w, num, (high, low) in zip(rows_b, weights, nums, peaks):
            den_high, den_low = split_in_two(jnp.sum(w, axis=1, keepdims=True))
            stats = jnp.where(
                stat_lane < 64,
                jnp.where(stat_lane < 32, high, low),
                jnp.where(stat_lane < 96, den_high, den_low),
            )
            att_out[b] = jnp.concatenate([num, stats], axis=0).astype(BF16)
        for b in rows_b:
            send_row(2, b, att_out, att_in)
        return 0

    with jax.named_scope("attend"):
        lax.fori_loop(0, B // SIDE, attend, 0)

    @pl.when(serves)
    def _():
        take_rows(2, att_out, att_in)
        arrived = att_in[...].astype(F32)
        num, stats = arrived[:, 0 : MAPS * NH], arrived[:, MAPS * NH : 2 * MAPS * NH]
        peak = stats[:, :, 0:1] + stats[:, :, 32:33]
        den = stats[:, :, 64:65] + stats[:, :, 96:97]
        own = own_rows[0][:, 0:1]
        highest = jnp.maximum(jnp.max(peak, axis=0), own)
        scale = jnp.exp(peak - highest[None])
        own_weight = jnp.exp(own - highest)
        own_round = own_weight.astype(BF16).astype(F32)
        total = jnp.sum(scale * den, axis=0) + own_weight
        weighted = jnp.sum(scale * num, axis=0) + own_round * own_rows[1]
        mixed = weighted / total
        head = lax.broadcasted_iota(jnp.int32, (NH, LANES), 0)
        its_lanes = lax.broadcasted_iota(jnp.int32, (NH, LANES), 1) == head * (LANES // NH)
        lam_rows = jnp.sum(jnp.where(its_lanes, own_rows[2][0:NH], 0.0), axis=1, keepdims=True)
        mixed = mixed[0:NH] - lam_rows * mixed[NH : 2 * NH]
        inv = lax.rsqrt(jnp.mean(mixed * mixed, axis=1, keepdims=True) + EPSILON)
        normed = mixed * inv * v_head_gain[...]
        head_row[...] = jnp.concatenate([normed, jnp.zeros((NH, LANES), F32)], axis=0).astype(BF16)
        share_row(2, head_row, head_all)

    take_all(2, att_out, short_rows, head_all)
    attended = as_lhs(head_all, NH)
    copies[8].wait()
    part = jnp.dot(attended, v_output[...], preferred_element_type=F32)
    second = (first + tp_sum(2, part)).astype(BF16).astype(F32)

    part = gated_units(1, second, v_gain3, v_gate2, v_up2, v_down2, copies[9:12])
    last = second + 0.5 * tp_sum(3, part)
    own_columns = lax.rem(LANES - t * columns, LANES)
    result[...] = pltpu.roll(last, own_columns, 1)[:, 0:columns].astype(BF16)


def on_device(KV, TP):
    def run(
        tokens,
        first_gain,
        first_gate,
        first_up,
        first_down,
        mixer_gain,
        w_query,
        w_key,
        w_value,
        w_output,
        lam_heads,
        head_gain,
        key_cache,
        value_cache,
        lengths,
        last_gain,
        last_gate,
        last_up,
        last_down,
    ):
        B, POS, NH, _ = key_cache.shape
        FB = first_gate.shape[1] // LANES
        FH = FB + 1
        HR = -(-FH // 8) * 8
        WIDTH = w_query.shape[0] * KV
        dims = (KV, TP, B, NH, FB, POS, WIDTH)
        far = pl.BlockSpec(memory_space=pl.ANY)
        smem = pl.BlockSpec(memory_space=pltpu.SMEM)
        flat_keys = key_cache.reshape(B, POS * NH, LANES)
        flat_values = value_cache.reshape(B, POS * NH, LANES)
        large = (first_gate, first_up, first_down, w_query, w_key, w_value, w_output)
        large += (flat_keys, flat_values, last_gate, last_up, last_down)
        return pl.pallas_call(
            functools.partial(layer_kernel, dims),
            out_shape=jax.ShapeDtypeStruct(tokens.shape, BF16),
            in_specs=[far] * 5 + [smem] * 2 + [far] * 12,
            out_specs=pl.BlockSpec(memory_space=pltpu.VMEM),
            scratch_shapes=[
                *(pltpu.VMEM(a.shape, a.dtype) for a in large),
                pltpu.VMEM(tokens.shape, BF16),
                *(pltpu.VMEM((1, LANES), F32) for _ in range(4)),
                pltpu.SemaphoreType.DMA((17,)),
                pltpu.VMEM((4, TP, B, LANES), BF16),
                pltpu.SemaphoreType.DMA((4,)),
                pltpu.SemaphoreType.DMA((4,)),
                pltpu.VMEM((max(2 * FH, 4 * NH) * B, LANES), F32),
                pltpu.VMEM((max(HR, 2 * NH) * B, LANES), F32),
                pltpu.VMEM((2, B, 2 * FH, LANES), BF16),
                pltpu.VMEM((2, KV, 2 * FH, LANES), BF16),
                pltpu.VMEM((B, 4 * NH, LANES), BF16),
                pltpu.VMEM((KV, 4 * NH, LANES), BF16),
                pltpu.VMEM((B, 4 * NH, LANES), BF16),
                pltpu.VMEM((KV, 4 * NH, LANES), BF16),
                pltpu.VMEM((2, HR, LANES), BF16),
                pltpu.VMEM((2, B, HR, LANES), BF16),
                pltpu.VMEM((2 * NH, LANES), BF16),
                pltpu.VMEM((B, 2 * NH, LANES), BF16),
                pltpu.VMEM((2 * NH, LANES), BF16),
                pltpu.VMEM((B, 2 * NH, LANES), BF16),
                pltpu.VMEM((3, 2 * NH, LANES), F32),
                pltpu.VMEM((KV, HR, LANES), BF16),
                pltpu.VMEM((KV, 2 * NH, LANES), BF16),
                pltpu.SemaphoreType.DMA((4,)),
                pltpu.SemaphoreType.DMA((4,)),
                pltpu.SemaphoreType.DMA((4,)),
                pltpu.SemaphoreType.DMA((4,)),
            ],
            compiler_params=pltpu.CompilerParams(collective_id=0, has_side_effects=True),
        )(
            tokens,
            first_gain.reshape(1, LANES),
            mixer_gain.reshape(1, LANES),
            last_gain.reshape(1, LANES),
            head_gain.reshape(1, LANES),
            lam_heads,
            lengths,
            first_gate,
            first_up,
            first_down,
            w_query,
            w_key,
            w_value,
            w_output,
            flat_keys,
            flat_values,
            last_gate,
            last_up,
            last_down,
        )

    return run


def solution(mesh):
    return jax.shard_map(
        on_device(mesh.shape["kv"], mesh.shape["tp"]),
        mesh=mesh,
        in_specs=(
            P(None, ("kv", "tp")),
            P("kv"),
            P("kv", "tp"),
            P("kv", "tp"),
            P("tp", "kv"),
            P("kv"),
            P("kv", "tp"),
            P("kv", "tp"),
            P("kv", "tp"),
            P("tp", "kv"),
            P("tp"),
            P(),
            P(None, "kv", "tp", None),
            P(None, "kv", "tp", None),
            P(),
            P("kv"),
            P("kv", "tp"),
            P("kv", "tp"),
            P("tp", "kv"),
        ),
        out_specs=P(None, ("kv", "tp")),
        check_vma=False,
    )
```
